128 devices in a mesh: rep: 2 (over z_hi), fs: 32 (over z_lo, y, x), tp: 2 (over core).
Axes of the slice: x: 4, y: 4, z: 4 (z_hi: 2, z_lo: 2; z = z_hi * 2 + z_lo), core: 2. Of those that a mesh axis runs over, the one named last changes fastest.
Arguments:
- hidden_in: bfloat16 [49152, 2048], P(('rep', 'fs', 'tp')), may hold values from -6 to 6
- norm_gain: float32 [2048], replicated, may hold values from 0.1 to 1.9
- up_weight: float32 [2048, 8192], P('fs', 'tp'), may hold values from -0.125 to 0.125
- up_scale: float32 [8192], P('tp'), may hold values from 0.5 to 2
- down_weight: float32 [8192, 2048], P('tp', 'fs'), may hold values from -0.0625 to 0.0625
- down_scale: float32 [2048], replicated, may hold values from 0.5 to 2
Outputs:
- layer_out: bfloat16 [49152, 2048], P(('rep', 'fs', 'tp'))
The draws below stay inside these ranges and needn't reach their ends.
All inputs are finite; a program needn't handle non-finite values.
Results may differ from the reference program's by a relative error of at most 0.0085.
Values may be sent and summed in bfloat16 or wider, within the bound.
A program may use at most 128 MiB of HBM per device.

```python
import math
import jax
import jax.numpy as jnp
from jax import lax

D = 2048
FF = 8192
TOKENS = 49152
N_TP = 2


def shard_levels(rng, shape, split, smallest, high):
    def one(dim, parts):
        draws = jax.random.uniform(jax.random.fold_in(jax.random.fold_in(rng, 6), dim), (parts,), jnp.float32, smallest / len(split), high / len(split))
        return jnp.repeat(jnp.exp(draws), shape[dim] // parts).reshape((-1,) + (1,) * (len(shape) - dim - 1))

    level = one(*split[0])
    for cut in split[1:]:
        level = level * one(*cut)
    return level


def normal_values(stream_key, shape, deviation, most, pieces=(), kind=jnp.bfloat16):
    level = shard_levels(stream_key, shape, pieces, -0.22, 0.18) if pieces else 1.0
    values = jax.random.normal(stream_key, shape, jnp.float32) * deviation * level
    return jnp.minimum(jnp.maximum(values, -most), most).astype(kind)


def setup_inputs(seed: int = 0) -> dict:
    seeds = jax.random.split(jax.random.key(seed), 7)
    return {
        "hidden_in": normal_values(seeds[0], (TOKENS, D), 1.0, 6.0, ((0, 128),)),
        "norm_gain": jnp.clip(1.0 + 0.18 * jax.random.normal(seeds[1], (D,), jnp.float32), 0.1, 1.9),
        "up_weight": normal_values(seeds[2], (D, FF), D ** -0.5, 0.125, ((0, 32), (1, 2)), jnp.float32),
        "up_scale": jnp.clip(jnp.exp(math.log(2.0) - 1.3862944 * jax.random.uniform(seeds[3], (FF,), jnp.float32) ** shard_levels(seeds[3], (FF,), ((0, 2),), -0.2, 0.2)), 0.5, 2.0),
        "down_weight": normal_values(seeds[4], (FF, D), FF ** -0.5, 0.0625, ((0, 2), (1, 32)), jnp.float32),
        "down_scale": jnp.clip(jnp.exp(jax.random.uniform(seeds[5], (D,), jnp.float32, math.log(0.5), math.log(2.0))), 0.5, 2.0),
    }


def reference(hidden_in, norm_gain, up_weight, up_scale, down_weight, down_scale):
    up_low = up_weight.astype(jnp.bfloat16)
    down_low = down_weight.astype(jnp.bfloat16)
    block = math.gcd(2048, TOKENS)
    width = FF // N_TP

    def one_block(start):
        rows = lax.dynamic_slice_in_dim(hidden_in, start, block, 0).astype(jnp.float32)
        normed = (rows * lax.rsqrt(lax.optimization_barrier(jnp.mean(rows * rows, axis=1, keepdims=True)) + 1e-06) * norm_gain).astype(jnp.bfloat16)
        pre = jnp.dot(normed, up_low, preferred_element_type=jnp.float32) * up_scale
        act = jnp.square(jnp.maximum(pre, 0.0)).astype(jnp.bfloat16)
        total = jnp.zeros((block, D), jnp.float32)
        for index in range(N_TP):
            part = jnp.dot(act[:, index * width:(index + 1) * width], down_low[index * width:(index + 1) * width], preferred_element_type=jnp.float32).astype(jnp.bfloat16)
            part = lax.optimization_barrier(part)
            total = total + part.astype(jnp.float32)
        return (total * down_scale).astype(jnp.bfloat16)
    starts = jnp.arange(0, TOKENS, block, dtype=jnp.int32)
    outs = lax.map(one_block, starts)
    return outs.reshape(TOKENS, D)
```

```python
import jax
import jax.numpy as jnp
from jax import lax
from jax.experimental import pallas as pl
from jax.experimental.pallas import tpu as pltpu
from jax.sharding import PartitionSpec as P

F32, BF16 = jnp.float32, jnp.bfloat16
ROWS, D, Q, GROUP, BLOCK = 384, 2048, 2048, 256, 64
HALF = Q // 2
STEP = ((1, 0, 0), (3, 0, 0), (0, 1, 0), (0, 3, 0), (0, 0, 1))
ORDER = (
    ((0, 0), (0, 1), (1, 0), (3, 0), (1, 1), (3, 1), (2, 0), (2, 1)),
    ((0, 0), (0, 1), (3, 0), (1, 0), (3, 1), (1, 1), (2, 0), (2, 1)),
)
PLAN = (
    (0,0,0,1,0,0,0), (0,0,1,1,0,0,0), (0,0,1,3,0,0,1), (0,0,0,3,0,0,1), (0,0,1,0,1,0,2), (0,0,0,0,1,0,2),
    (0,0,0,0,3,0,3), (0,0,1,0,3,0,3), (0,0,0,0,0,1,4), (0,0,1,0,0,1,4), (0,1,1,1,0,0,0), (0,1,0,3,0,0,1),
    (0,1,0,0,3,0,3), (0,1,0,0,0,1,4), (0,0,0,1,1,0,2), (0,0,0,1,0,1,0), (0,0,0,3,0,1,1), (0,0,0,0,1,1,2),
    (0,0,1,3,3,0,3), (0,0,1,0,1,1,4), (1,0), (0,1,0,1,0,0,0), (0,0,1,2,0,0,1), (0,0,0,0,2,0,2), (0,0,1,0,3,1,3),
    (0,0,1,1,0,1,4), (0,0,0,2,1,0,0), (0,0,1,3,1,0,1), (0,0,0,1,2,0,2), (0,0,0,3,3,0,3), (0,0,0,1,1,1,4), (1,1),
    (0,0,1,1,1,1,0), (0,0,0,2,0,1,1), (0,0,1,0,2,1,2), (0,0,0,1,3,0,3), (0,0,1,3,3,1,4), (1,2), (0,0,1,1,3,1,0),
    (0,0,0,3,1,1,1), (0,0,1,2,1,0,2), (0,0,1,3,2,0,3), (0,0,1,2,0,1,4), (0,0,0,2,2,0,0), (0,0,0,2,3,0,1),
    (0,0,0,1,2,1,2), (0,0,0,2,0,0,3), (0,0,1,3,1,1,4), (1,3), (0,1,1,2,0,0,0), (0,0,1,2,3,0,1), (0,0,1,3,0,1,2),
    (0,0,0,0,3,1,3), (0,0,0,1,3,1,4), (1,4), (0,0,1,0,2,0,0), (0,0,1,1,1,0,1), (0,0,1,2,1,1,2), (0,0,0,3,3,1,3),
    (0,0,0,3,1,0,4), (2,0,0), (0,0,0,3,2,0,0), (0,0,0,2,1,1,1), (0,0,1,2,2,0,2), (0,0,0,2,3,1,3), (0,0,1,1,3,0,4),
    (2,0,1), (1,5), (2,1,0), (0,0,0,2,2,1,0), (0,1,0,2,0,0,1), (0,0,1,1,2,1,2), (0,0,1,2,3,1,3), (0,0,0,0,2,1,4),
    (2,1,1), (1,6), (2,2,0), (0,0,1,1,2,0,0), (0,1,0,3,0,1,1), (0,0,1,2,2,1,2), (0,0,0,3,2,1,3), (0,0,1,3,2,1,4),
    (2,2,1), (2,3,0), (0,1,0,1,0,1,0), (0,1,1,3,0,0,1), (0,1,0,3,1,0,2), (0,1,1,2,3,0,3), (0,1,1,2,0,1,4), (2,3,1),
    (1,7), (2,4,0), (2,4,1), (0,1,0,1,3,0,0), (0,1,0,2,1,0,2), (0,1,0,3,3,0,3), (0,1,1,0,0,1,4), (2,5,0), (2,5,1),
    (0,1,0,2,0,1,1), (2,6,0), (0,1,1,1,1,0,2), (0,1,0,2,3,0,3), (2,6,1), (2,7,0), (0,1,1,3,3,0,0), (0,1,1,1,0,1,1),
    (0,1,1,3,0,1,4), (2,7,1), (0,1,0,0,1,0,0), (0,1,1,1,3,0,1), (0,1,1,3,1,0,2), (0,1,1,0,3,0,3), (0,1,1,2,3,1,4),
    (3,0), (4,0), (0,1,0,1,1,0,1), (0,1,0,2,1,1,2), (0,1,0,0,3,1,3), (0,1,0,3,3,1,4), (5,0), (0,1,1,2,1,0,0), (3,1),
    (0,1,0,3,2,0,2), (0,1,1,0,3,1,3), (0,1,1,3,3,1,4), (4,1), (5,1), (0,1,1,0,1,0,0), (0,1,1,1,3,1,1), (3,2),
    (0,1,1,0,1,1,2), (0,1,1,0,2,0,3), (0,1,0,0,1,1,4), (4,2), (5,2), (6,0), (0,1,0,1,3,1,0), (0,1,0,2,3,1,1),
    (0,1,0,3,1,1,0), (0,1,0,1,2,0,2), (0,1,0,0,2,1,3), (0,1,1,1,1,1,4), (0,1,0,2,2,0,1), (3,3), (0,1,1,3,1,1,2),
    (0,1,1,2,2,0,3), (0,1,1,2,1,1,4), (6,1), (4,3), (5,3), (0,1,0,1,1,1,0), (0,1,1,3,2,0,1), (3,4), (0,1,1,1,2,0,0),
    (0,1,1,0,2,1,3), (4,4), (5,4), (6,2), (0,1,0,0,2,0,1), (0,1,0,2,2,1,4), (0,1,0,3,2,1,1), (0,1,1,1,2,1,3),
    (0,1,0,1,2,1,2), (0,1,1,3,2,1,2), (0,1,1,2,2,1,4), (3,5), (4,5), (5,5), (6,3), (3,6), (4,6), (5,6), (6,4), (3,7),
    (4,7), (6,5), (5,7), (6,6), (6,7),
)


def kernel(hidden, gain, up, up_scale, down, down_scale, out, hbuf, ubuf, dbuf, w, x, acc, act, pbuf, sibp, mine, own,
           zbuf, zrecv, obuf, in_sem, ag_send, ag_recv, tok_send, tok_recv, par_send, par_recv, out_sem):
    rep, fs, core = lax.axis_index("rep"), lax.axis_index("fs"), lax.axis_index("tp")
    lo, yy, xx = fs // 16, (fs // 4) % 4, fs % 4
    turn = 1 + 2 * core

    def at(px, py, plo):
        return (plo * 4 + py) * 4 + px

    def neighbour(d):
        dx, dy, dz = STEP[d]
        return {"fs": at((xx + turn * dx) % 4, (yy + dy) % 4, (lo + dz) % 2)}

    sibling = {"tp": 1 - core}
    across = {"rep": 1 - rep, "fs": at(xx, yy, 1 - lo)}

    loads = [
        pltpu.make_async_copy(up.at[:, pl.ds(pl.multiple_of(rep * Q, Q), Q)], ubuf, in_sem.at[0]),
        pltpu.make_async_copy(hidden, hbuf, in_sem.at[1]),
        pltpu.make_async_copy(down.at[:, pl.ds(pl.multiple_of(rep * Q, Q), Q)], dbuf, in_sem.at[2]),
    ]
    for load in loads:
        load.start()
    barrier = pltpu.get_barrier_semaphore()
    for peer in [neighbour(d) for d in range(5)] + [sibling, across]:
        pl.semaphore_signal(barrier, inc=1, device_id=peer, device_id_type=pl.DeviceIdType.MESH)

    me_rows = pl.ds(pl.multiple_of(fs * BLOCK, BLOCK), BLOCK)
    loads[0].wait()
    w[0, me_rows, :] = ubuf[...].astype(BF16)
    loads[2].wait()
    w[1, me_rows, :] = dbuf[...].astype(BF16)
    pl.semaphore_wait(barrier, 7)

    def block_rows(o):
        return pl.ds(pl.multiple_of(at((xx + 4 - (turn * o[0]) % 4) % 4, (yy + 4 - o[1]) % 4, (lo + o[2]) % 2) * BLOCK, BLOCK), BLOCK)

    def remote(src, dst, send, recv, peer):
        return pltpu.make_async_remote_copy(src_ref=src, dst_ref=dst, send_sem=send, recv_sem=recv, device_id=peer,
                                            device_id_type=pl.DeviceIdType.MESH)

    def number(phase, half, o):
        return ((phase * 2 + half) * 2 + o[2]) * 16 + o[1] * 4 + o[0]

    waited = set()

    def block_copy(phase, half, o, d):
        s = STEP[d]
        held = ((o[0] - s[0]) % 4, (o[1] - s[1]) % 4, (o[2] - s[2]) % 2)
        ref = w.at[phase, block_rows(held), pl.ds(half * HALF, HALF)]
        return remote(ref, ref, ag_send.at[phase], ag_recv.at[number(phase, half, o)], neighbour(d))

    def need(phase, half, o):
        if o != (0, 0, 0) and (phase, half, o) not in waited:
            waited.add((phase, half, o))
            ref = w.at[phase, block_rows(o), pl.ds(half * HALF, HALF)]
            remote(ref, ref, ag_send.at[phase], ag_recv.at[number(phase, half, o)], sibling).wait_recv()

    def send(phase, half, o, d):
        s = STEP[d]
        held = ((o[0] - s[0]) % 4, (o[1] - s[1]) % 4, (o[2] - s[2]) % 2)
        need(phase, half, held)
        block_copy(phase, half, o, d).start()

    def need_group(phase, g):
        y, z = ORDER[phase][g]
        for half in range(2):
            for a in range(4):
                need(phase, half, (a, y, z))

    def group(phase, g, far=0):
        y, z = ORDER[phase][g]
        return ((lo + far + z) % 2) * 4 + (yy + 4 - y) % 4

    def columns(a):
        return pl.ds(pl.multiple_of(a * GROUP, GROUP), GROUP)

    sib_rows, sib_far_rows, my_rows, far_rows = (pl.ds(i * ROWS, ROWS) for i in range(4))

    def token_far(g):
        a = group(0, g, 1)
        return remote(x.at[a, my_rows], x.at[a, far_rows], tok_send.at[0], tok_recv.at[0, g], across)

    def token_far_in(g):
        a = group(0, g)
        return remote(x.at[a, my_rows], x.at[a, far_rows], tok_send.at[0], tok_recv.at[0, g], across)

    def token_near(g):
        a = group(0, g)
        return remote(x.at[a, my_rows], x.at[a, sib_rows], tok_send.at[1], tok_recv.at[1, g], sibling)

    def token_relay(g):
        a = group(0, g)
        return remote(x.at[a, far_rows], x.at[a, sib_far_rows], tok_send.at[2], tok_recv.at[2, g], sibling)

    def near_part(g):
        return remote(pbuf.at[g], sibp.at[g], par_send.at[0], par_recv.at[0, g], sibling)

    def far_part(g):
        return remote(zbuf.at[g], zrecv.at[g], par_send.at[1], par_recv.at[1, g], across)

    plan = list(PLAN)
    while plan[0][0] == 0:
        send(plan[0][1], plan[0][2], plan[0][3:6], plan[0][6])
        plan.pop(0)

    loads[1].wait()

    @pl.loop(0, ROWS // 32)
    def _(i):
        rows = hbuf[pl.ds(i * 32, 32), :].astype(F32)
        inv = lax.rsqrt(jnp.mean(rows * rows, axis=1, keepdims=True) + 1e-06)
        normed = (rows * inv * gain[...]).astype(BF16)
        for a in range(8):
            x[a, pl.ds(2 * ROWS + i * 32, 32), :] = normed[:, a * GROUP:(a + 1) * GROUP]

    for g in range(8):
        token_far(g).start()
        token_near(g).start()

    half_scale = up_scale.at[:, pl.ds(pl.multiple_of(rep * Q, Q), Q)]

    def up_product(g, part):
        if part == 0:
            need_group(0, g)
            token_near(g).wait_recv()
            token_relay(g).wait_recv()
        a = group(0, g)

        @pl.loop(part * 4, part * 4 + 4)
        def _(n):
            tokens = x[a]
            total = jnp.dot(tokens, w[0, columns(a), columns(n)], preferred_element_type=F32)
            if g > 0:
                total = total + acc[n]
            if g < 7:
                acc[n] = total
            else:
                act[:, columns(n)] = jnp.square(jnp.maximum(total * half_scale[:, columns(n)], 0.0)).astype(BF16)

    def product(rows, a):
        return lax.dot_general(act[rows, :], w[1, columns(a), :], (((1,), (1,)), ((), ())), preferred_element_type=F32)

    def down_first(g):
        need_group(1, g)
        a = group(1, g)

        @pl.loop(0, 2)
        def _(m):
            rows = pl.ds(pl.multiple_of(m * ROWS, ROWS), ROWS)
            pbuf[g, rows, :] = product(rows, a).astype(BF16)

        near_part(g).start()

    def down_second(g):
        a = group(1, g)

        @pl.loop(0, 2)
        def _(m):
            own[m] = product(pl.ds(pl.multiple_of((m + 2) * ROWS, ROWS), ROWS), a)

    def chip_sum(g):
        a = group(1, g)
        near_part(g).wait_recv()
        zbuf[g] = (own[1] + sibp[g, pl.ds(ROWS, ROWS), :].astype(F32)).astype(BF16)
        far_part(g).start()
        mine[a] = own[0] + sibp[g, pl.ds(0, ROWS), :].astype(F32)

    def out_copy(g):
        return pltpu.make_async_copy(obuf.at[g], out.at[:, columns(group(1, g, 1))], out_sem.at[g])

    def output(g):
        a = group(1, g, 1)
        far_part(g).wait_recv()
        obuf[g] = ((mine[a] + zrecv[g].astype(F32)) * down_scale[:, columns(a)]).astype(BF16)
        out_copy(g).start()

    for step in plan:
        kind, arg = step[0], step[1]
        if kind == 0:
            send(arg, step[2], step[3:6], step[6])
        elif kind == 1:
            token_far_in(arg).wait_recv()
            token_relay(arg).start()
        elif kind == 2:
            up_product(arg, step[2])
        elif kind == 3:
            down_first(arg)
        elif kind == 4:
            down_second(arg)
        elif kind == 5:
            chip_sum(arg)
        else:
            output(arg)

    for phase in range(2):
        sent = w.at[phase, pl.ds(0, 31 * BLOCK), :]
        remote(sent, sent, ag_send.at[phase], ag_recv.at[0], sibling).wait_send()
    for i in range(3):
        sent = x.at[:, pl.ds(0, ROWS)]
        remote(sent, sent, tok_send.at[i], tok_recv.at[0, 0], sibling).wait_send()
    remote(pbuf, pbuf, par_send.at[0], par_recv.at[0, 0], sibling).wait_send()
    remote(zbuf, zbuf, par_send.at[1], par_recv.at[0, 0], sibling).wait_send()
    for g in range(8):
        out_copy(g).wait()


def body(hidden_in, norm_gain, up_weight, up_scale, down_weight, down_scale):
    vmem, anywhere = pl.BlockSpec(memory_space=pltpu.VMEM), pl.BlockSpec(memory_space=pl.ANY)
    dma = pltpu.SemaphoreType.DMA
    return pl.pallas_call(
        kernel,
        out_shape=jax.ShapeDtypeStruct((ROWS, D), BF16),
        in_specs=[anywhere, vmem, anywhere, vmem, anywhere, vmem],
        out_specs=anywhere,
        scratch_shapes=[
            pltpu.VMEM((ROWS, D), BF16),
            pltpu.VMEM((BLOCK, Q), F32),
            pltpu.VMEM((BLOCK, Q), F32),
            pltpu.VMEM((2, D, Q), BF16),
            pltpu.VMEM((8, 4 * ROWS, GROUP), BF16),
            pltpu.VMEM((8, 4 * ROWS, GROUP), F32),
            pltpu.VMEM((4 * ROWS, Q), BF16),
            pltpu.VMEM((8, 2 * ROWS, GROUP), BF16),
            pltpu.VMEM((8, 2 * ROWS, GROUP), BF16),
            pltpu.VMEM((8, ROWS, GROUP), F32),
            pltpu.VMEM((2, ROWS, GROUP), F32),
            pltpu.VMEM((8, ROWS, GROUP), BF16),
            pltpu.VMEM((8, ROWS, GROUP), BF16),
            pltpu.VMEM((8, ROWS, GROUP), BF16),
            dma((3,)),
            dma((2,)),
            dma((128,)),
            dma((3,)),
            dma((3, 8)),
            dma((2,)),
            dma((2, 8)),
            dma((8,)),
        ],
        compiler_params=pltpu.CompilerParams(collective_id=0, has_side_effects=True, vmem_limit_bytes=67043328),
        name="ffn",
    )(hidden_in, norm_gain.reshape(1, -1), up_weight, up_scale.reshape(1, -1), down_weight.T, down_scale.reshape(1, -1))


def solution(mesh):
    placed = (P(("rep", "fs", "tp"), None), P(), P("fs", "tp"), P("tp"), P("tp", "fs"), P())
    return jax.shard_map(
        body, mesh=mesh, in_specs=placed, out_specs=P(("rep", "fs", "tp"), None), check_vma=False
    )
```

```python
import jax
import jax.numpy as jnp
from jax import lax
from jax.experimental import pallas as pl
from jax.experimental.pallas import tpu as pltpu
from jax.sharding import PartitionSpec as P

F32, BF16 = jnp.float32, jnp.bfloat16
ROWS, D, Q, GROUP, BLOCK = 384, 2048, 2048, 256, 64
HALF, WIDE = Q // 2, Q // 2
STEP = ((1, 0, 0), (3, 0, 0), (0, 1, 0), (0, 3, 0), (0, 0, 1))
ORDER = (
    ((0, 0), (0, 1), (1, 0), (3, 0), (1, 1), (3, 1), (2, 0), (2, 1)),
    ((0, 0), (0, 1), (3, 0), (1, 0), (3, 1), (1, 1), (2, 0), (2, 1)),
)
PLAN = (
    (0,0,0,1,0,0,0), (0,0,1,1,0,0,0), (0,0,1,3,0,0,1), (0,0,0,3,0,0,1), (0,0,1,0,1,0,2), (0,0,0,0,1,0,2),
    (0,0,1,0,3,0,3), (0,0,0,0,3,0,3), (0,0,0,0,0,1,4), (0,1,1,0,0,1,4), (0,1,0,1,0,0,0), (0,1,0,3,0,0,1),
    (0,1,1,0,3,0,3), (0,0,0,1,1,0,2), (0,0,1,3,0,1,4), (0,0,0,1,0,1,0), (0,0,1,2,0,0,1), (0,0,1,3,1,0,2),
    (0,0,0,1,3,0,3), (0,0,1,0,1,1,4), (0,0,0,2,0,0,0), (0,0,0,3,1,0,1), (0,0,1,1,1,0,2), (1,0), (0,0,1,0,2,0,3),
    (0,0,1,1,0,1,4), (0,0,0,2,1,0,0), (0,0,1,2,0,1,1), (0,0,0,1,2,0,2), (0,0,1,3,3,0,3), (0,0,0,3,0,1,4), (1,1),
    (0,0,1,1,1,1,0), (0,0,1,2,1,0,1), (0,0,0,1,1,1,2), (0,0,1,0,0,1,3), (0,0,0,0,3,1,4), (2,0,0), (0,0,1,1,2,0,0),
    (0,1,1,3,0,0,1), (0,0,0,3,2,0,2), (0,0,1,2,3,0,3), (0,0,0,3,1,1,4), (1,2), (2,0,1), (0,0,0,2,0,1,0),
    (0,0,0,0,2,0,1), (0,0,1,2,1,1,2), (0,0,0,3,3,1,3), (0,0,0,2,1,1,4), (1,3), (0,0,0,2,3,0,0), (0,1,0,2,0,0,1),
    (0,0,1,0,2,1,2), (0,0,1,1,3,1,3), (0,0,0,1,3,1,4), (0,0,0,0,1,1,0), (0,0,1,1,3,0,1), (1,4), (0,0,0,3,3,0,2),
    (0,0,0,0,2,1,3), (0,0,1,1,2,1,4), (2,1,0), (0,0,1,3,1,1,0), (0,1,1,2,0,0,1), (0,0,1,2,2,0,2), (0,0,0,2,3,1,3),
    (0,0,1,2,3,1,4), (2,1,1), (1,5), (2,2,0), (0,1,1,1,3,0,0), (0,0,1,3,2,1,1), (0,0,1,0,3,1,2), (0,0,1,3,2,0,3),
    (0,0,1,3,3,1,4), (2,2,1), (2,3,0), (0,0,0,1,2,1,0), (0,1,1,3,0,1,1), (0,0,0,2,2,1,2), (0,0,0,2,2,0,3),
    (0,1,0,3,0,1,4), (1,6), (2,3,1), (2,4,0), (0,0,1,2,2,1,0), (0,1,1,1,0,0,1), (0,0,0,3,2,1,2), (0,1,0,3,3,0,3),
    (0,1,0,1,0,1,4), (2,4,1), (1,7), (2,5,0), (0,1,1,2,3,0,0), (0,1,0,3,1,0,2), (0,1,0,2,3,0,3), (0,1,1,0,3,1,4),
    (2,5,1), (0,1,1,2,0,1,1), (2,6,0), (0,1,0,0,0,1,0), (0,1,0,2,0,1,1), (0,1,1,3,1,0,2), (0,1,0,0,3,0,3), (2,6,1),
    (0,1,1,1,0,1,4), (2,7,0), (0,1,1,1,1,0,2), (0,1,1,3,3,0,3), (0,1,0,3,3,1,4), (3,0), (0,1,0,0,1,0,0),
    (0,1,0,1,3,0,1), (2,7,1), (0,1,1,1,3,1,0), (0,1,0,2,1,0,1), (0,1,1,2,1,0,2), (0,1,1,3,3,1,3), (0,1,0,3,1,1,4),
    (4,0), (5,0), (0,1,1,2,1,1,2), (0,1,0,2,3,1,3), (3,1), (6,0), (5,1), (0,1,0,1,1,0,0), (0,1,0,0,3,1,0),
    (0,1,1,0,1,0,1), (0,1,1,1,2,0,2), (0,1,0,0,2,0,3), (0,1,0,1,3,1,4), (4,1), (3,2), (6,1), (5,2), (0,1,0,0,1,1,0),
    (0,1,1,2,3,1,1), (0,1,1,3,2,0,2), (0,1,0,1,2,0,3), (0,1,0,2,1,1,4), (4,2), (7,0), (6,2), (0,1,1,1,1,1,1),
    (0,1,0,1,1,1,4), (0,1,1,2,2,1,2), (3,3), (0,1,1,3,1,1,0), (0,1,0,2,2,1,3), (0,1,1,0,1,1,4), (5,3),
    (0,1,0,3,2,0,1), (4,3), (0,1,1,2,2,0,3), (7,1), (3,4), (0,1,1,0,2,0,1), (0,1,1,1,2,1,4), (6,3), (5,4),
    (0,1,0,2,2,0,0), (0,1,0,0,2,1,2), (4,4), (0,1,1,3,2,1,4), (6,4), (7,2), (0,1,0,3,2,1,0), (0,1,0,1,2,1,1),
    (0,1,1,0,2,1,2), (3,5), (5,5), (4,5), (3,6), (6,5), (5,6), (4,6), (3,7), (6,6), (5,7), (4,7), (7,3), (7,4),
    (6,7), (7,5), (7,6), (7,7),
)


def kernel(hidden, gain, up, up_scale, down, down_scale, out, hbuf, ubuf, dbuf, w, x, acc, act, pbuf, sibp, own, zbuf, zrecv,
           in_sem, ag_send, ag_recv, tok_send, tok_recv, par_send, par_recv):
    rep, fs, core = lax.axis_index("rep"), lax.axis_index("fs"), lax.axis_index("tp")
    lo, yy, xx = fs // 16, (fs // 4) % 4, fs % 4
    turn = 1 + 2 * core

    def at(px, py, plo):
        return (plo * 4 + py) * 4 + px

    def neighbour(d):
        dx, dy, dz = STEP[d]
        return {"fs": at((xx + turn * dx) % 4, (yy + dy) % 4, (lo + dz) % 2)}

    sibling = {"tp": 1 - core}
    across = {"rep": 1 - rep, "fs": at(xx, yy, 1 - lo)}

    loads = [
        pltpu.make_async_copy(up.at[:, pl.ds(pl.multiple_of(rep * Q, Q), Q)], ubuf, in_sem.at[0]),
        pltpu.make_async_copy(hidden, hbuf, in_sem.at[1]),
        pltpu.make_async_copy(down.at[:, pl.ds(pl.multiple_of(rep * Q, Q), Q)], dbuf, in_sem.at[2]),
    ]
    for load in loads:
        load.start()
    barrier = pltpu.get_barrier_semaphore()
    for peer in [neighbour(d) for d in range(5)] + [sibling, across]:
        pl.semaphore_signal(barrier, inc=1, device_id=peer, device_id_type=pl.DeviceIdType.MESH)

    me_rows = pl.ds(pl.multiple_of(fs * BLOCK, BLOCK), BLOCK)
    loads[0].wait()
    w[0, me_rows, :] = ubuf[...].astype(BF16)
    loads[2].wait()
    w[1, me_rows, :] = dbuf[...].astype(BF16)
    pl.semaphore_wait(barrier, 7)

    def block_rows(o):
        return pl.ds(pl.multiple_of(at((xx + 4 - (turn * o[0]) % 4) % 4, (yy + 4 - o[1]) % 4, (lo + o[2]) % 2) * BLOCK, BLOCK), BLOCK)

    def remote(src, dst, send, recv, peer):
        return pltpu.make_async_remote_copy(src_ref=src, dst_ref=dst, send_sem=send, recv_sem=recv, device_id=peer,
                                            device_id_type=pl.DeviceIdType.MESH)

    def number(phase, half, o):
        return ((phase * 2 + half) * 2 + o[2]) * 16 + o[1] * 4 + o[0]

    waited = set()

    def block_copy(phase, half, o, d):
        s = STEP[d]
        held = ((o[0] - s[0]) % 4, (o[1] - s[1]) % 4, (o[2] - s[2]) % 2)
        ref = w.at[phase, block_rows(held), pl.ds(half * HALF, HALF)]
        return remote(ref, ref, ag_send.at[phase], ag_recv.at[number(phase, half, o)], neighbour(d))

    def need(phase, half, o):
        if o != (0, 0, 0) and (phase, half, o) not in waited:
            waited.add((phase, half, o))
            ref = w.at[phase, block_rows(o), pl.ds(half * HALF, HALF)]
            remote(ref, ref, ag_send.at[phase], ag_recv.at[number(phase, half, o)], sibling).wait_recv()

    def send(phase, half, o, d):
        s = STEP[d]
        held = ((o[0] - s[0]) % 4, (o[1] - s[1]) % 4, (o[2] - s[2]) % 2)
        need(phase, half, held)
        block_copy(phase, half, o, d).start()

    def need_group(phase, g):
        y, z = ORDER[phase][g]
        for half in range(2):
            for a in range(4):
                need(phase, half, (a, y, z))

    def group(phase, g, far=0):
        y, z = ORDER[phase][g]
        return ((lo + far + z) % 2) * 4 + (yy + 4 - y) % 4

    def columns(a):
        return pl.ds(pl.multiple_of(a * GROUP, GROUP), GROUP)

    sib_far_rows, far_rows, sib_rows, my_rows = (pl.ds(i * ROWS, ROWS) for i in range(4))

    def token_far(g):
        a = group(0, g, 1)
        return remote(x.at[a, my_rows], x.at[a, far_rows], tok_send.at[0], tok_recv.at[0, g], across)

    def token_far_in(g):
        a = group(0, g)
        return remote(x.at[a, my_rows], x.at[a, far_rows], tok_send.at[0], tok_recv.at[0, g], across)

    def token_near(g):
        a = group(0, g)
        return remote(x.at[a, my_rows], x.at[a, sib_rows], tok_send.at[1], tok_recv.at[1, g], sibling)

    def token_relay(g):
        a = group(0, g)
        return remote(x.at[a, far_rows], x.at[a, sib_far_rows], tok_send.at[2], tok_recv.at[2, g], sibling)

    def near_part(g, i):
        return remote(pbuf.at[2 * g + i, 0], sibp.at[g, i], par_send.at[0], par_recv.at[i, g], sibling)

    def far_part(g):
        return remote(zbuf.at[g], zrecv.at[g], par_send.at[1], par_recv.at[2, g], across)

    plan = list(PLAN)
    while plan[0][0] == 0 and STEP[plan[0][6]] == tuple(plan[0][3:6]):
        send(plan[0][1], plan[0][2], plan[0][3:6], plan[0][6])
        plan.pop(0)
    loads[1].wait()

    @pl.loop(0, ROWS // 32)
    def _(i):
        rows = hbuf[pl.ds(i * 32, 32), :].astype(F32)
        inv = lax.rsqrt(jnp.mean(rows * rows, axis=1, keepdims=True) + 1e-06)
        normed = (rows * inv * gain[...]).astype(BF16)
        for a in range(8):
            x[a, pl.ds(3 * ROWS + i * 32, 32), :] = normed[:, a * GROUP:(a + 1) * GROUP]

    for g in range(8):
        token_far(g).start()
    for g in range(8):
        token_near(g).start()

    half_scale = up_scale.at[:, pl.ds(pl.multiple_of(rep * Q, Q), Q)]

    def up_product(g, part):
        need_group(0, g)
        if part == 0:
            token_relay(g).wait_recv()
        else:
            token_near(g).wait_recv()
        a, rows = group(0, g), pl.ds(part * 2 * ROWS, 2 * ROWS)

        @pl.loop(0, 2)
        def _(n):
            wide = pl.ds(pl.multiple_of(n * WIDE, WIDE), WIDE)
            total = jnp.dot(x[a, rows, :], w[0, columns(a), wide], preferred_element_type=F32)
            if g > 0:
                total = total + acc[n, rows, :]
            if g < 7:
                acc[n, rows, :] = total
            else:
                act[rows, wide] = jnp.square(jnp.maximum(total * half_scale[:, wide], 0.0)).astype(BF16)

    def mine(a):
        return acc.at[0, pl.ds(pl.multiple_of((a % 4) * ROWS, ROWS), ROWS), columns(a // 4)]

    def products(first, a, keep):
        @pl.loop(0, 2)
        def _(i):
            rows = pl.ds(pl.multiple_of((first + i) * ROWS, ROWS), ROWS)
            part = lax.dot_general(act[rows, :], w[1, columns(a), :], (((1,), (1,)), ((), ())), preferred_element_type=F32)
            pbuf[keep, i] = part.astype(BF16)
            own[keep % 2, i] = part

    def down_far(g):
        need_group(1, g)
        products(0, group(1, g), 2 * g)
        near_part(g, 0).start()

    def sum_far(g):
        near_part(g, 0).wait_recv()
        zbuf[g] = (own[0, 1] + sibp[g, 0].astype(F32)).astype(BF16)
        far_part(g).start()

    def down_near(g):
        products(2, group(1, g), 2 * g + 1)
        near_part(g, 1).start()

    def output_sum(g):
        near_part(g, 1).wait_recv()
        mine(group(1, g))[...] = own[1, 1] + sibp[g, 1].astype(F32)

    def output(g):
        a = group(1, g, 1)
        far_part(g).wait_recv()
        out[:, columns(a)] = ((mine(a)[...] + zrecv[g].astype(F32)) * down_scale[:, columns(a)]).astype(BF16)

    for step in plan:
        kind, arg = step[0], step[1]
        if kind == 0:
            send(arg, step[2], step[3:6], step[6])
        elif kind == 1:
            token_far_in(arg).wait_recv()
            token_relay(arg).start()
        elif kind == 2:
            up_product(arg, step[2])
        elif kind == 3:
            down_far(arg)
        elif kind == 4:
            sum_far(arg)
        elif kind == 5:
            down_near(arg)
        elif kind == 6:
            output_sum(arg)
        else:
            output(arg)

    for phase in range(2):
        sent = w.at[phase, pl.ds(0, 31 * BLOCK), :]
        remote(sent, sent, ag_send.at[phase], ag_recv.at[0], sibling).wait_send()
    for i in range(3):
        sent = x.at[:, pl.ds(0, ROWS)]
        remote(sent, sent, tok_send.at[i], tok_recv.at[0, 0], sibling).wait_send()
    remote(sibp, sibp, par_send.at[0], par_recv.at[0, 0], sibling).wait_send()
    remote(zbuf, zbuf, par_send.at[1], par_recv.at[0, 0], sibling).wait_send()


def body(hidden_in, norm_gain, up_weight, up_scale, down_weight, down_scale):
    vmem, anywhere = pl.BlockSpec(memory_space=pltpu.VMEM), pl.BlockSpec(memory_space=pl.ANY)
    dma = pltpu.SemaphoreType.DMA
    return pl.pallas_call(
        kernel,
        out_shape=pltpu.VMEM((ROWS, D), BF16),
        in_specs=[anywhere, vmem, anywhere, vmem, anywhere, vmem],
        out_specs=vmem,
        scratch_shapes=[
            pltpu.VMEM((ROWS, D), BF16),
            pltpu.VMEM((BLOCK, Q), F32),
            pltpu.VMEM((BLOCK, Q), F32),
            pltpu.VMEM((2, D, Q), BF16),
            pltpu.VMEM((8, 4 * ROWS, GROUP), BF16),
            pltpu.VMEM((Q // WIDE, 4 * ROWS, WIDE), F32),
            pltpu.VMEM((4 * ROWS, Q), BF16),
            pltpu.VMEM((16, 2, ROWS, GROUP), BF16),
            pltpu.VMEM((8, 2, ROWS, GROUP), BF16),
            pltpu.VMEM((2, 2, ROWS, GROUP), F32),
            pltpu.VMEM((8, ROWS, GROUP), BF16),
            pltpu.VMEM((8, ROWS, GROUP), BF16),
            dma((3,)),
            dma((2,)),
            dma((128,)),
            dma((3,)),
            dma((3, 8)),
            dma((2,)),
            dma((3, 8)),
        ],
        compiler_params=pltpu.CompilerParams(collective_id=0, has_side_effects=True, vmem_limit_bytes=63000000),
        name="ffn",
    )(hidden_in, norm_gain.reshape(1, -1), up_weight, up_scale.reshape(1, -1), down_weight.T, down_scale.reshape(1, -1))


def solution(mesh):
    placed = (P(("rep", "fs", "tp"), None), P(), P("fs", "tp"), P("tp"), P("tp", "fs"), P())
    return jax.shard_map(
        body, mesh=mesh, in_specs=placed, out_specs=P(("rep", "fs", "tp"), None), check_vma=False
    )
```

```python
import jax
import jax.numpy as jnp
from jax import lax
from jax.experimental import pallas as pl
from jax.experimental.pallas import tpu as pltpu
from jax.sharding import PartitionSpec as P

F32, BF16 = jnp.float32, jnp.bfloat16
ROWS, D, Q, GROUP, BLOCK = 384, 2048, 2048, 256, 64
CHUNKS, WIDE = 2, Q // 2
CHUNK = Q // CHUNKS
STEP = ((1, 0, 0), (3, 0, 0), (0, 1, 0), (0, 3, 0), (0, 0, 1))
ORDER = (
    ((0, 0), (0, 1), (1, 0), (3, 0), (1, 1), (3, 1), (2, 0), (2, 1)),
    ((0, 0), (0, 1), (3, 0), (1, 0), (3, 1), (1, 1), (2, 0), (2, 1)),
)
PLAN = (
    (0,0,0,1,0,0,0), (0,0,0,3,0,0,1), (0,0,1,0,1,0,2), (0,0,0,0,3,0,3), (0,0,1,0,0,1,4), (0,0,1,1,0,0,0),
    (0,1,0,3,0,0,1), (0,0,0,0,1,0,2), (0,0,1,0,3,0,3), (0,0,0,3,0,1,4), (0,1,1,1,0,0,0), (0,0,1,3,1,0,1),
    (0,0,1,0,1,1,2), (0,0,0,1,3,0,3), (0,0,0,0,3,1,4), (0,0,1,2,0,0,0), (0,0,0,3,1,0,1), (0,0,1,1,1,0,2),
    (0,0,1,1,3,0,3), (1,0), (0,0,0,0,1,1,4), (0,0,0,2,3,0,0), (0,0,0,2,0,1,1), (0,0,1,0,2,1,2), (0,0,0,1,2,0,3),
    (1,1), (0,0,1,1,3,1,4), (0,0,1,3,0,0,0), (0,0,0,2,0,0,1), (0,0,0,3,2,0,2), (0,0,1,1,2,0,3), (0,0,1,2,1,0,0),
    (0,1,1,3,0,0,1), (0,0,0,3,3,0,3), (0,0,1,0,3,1,2), (0,0,0,1,2,1,4), (1,2), (0,0,1,0,2,0,4), (0,0,0,1,1,1,0),
    (0,0,0,0,2,0,1), (0,0,0,2,2,0,3), (0,0,1,1,0,1,2), (2,0,0,0), (0,0,1,3,0,1,4), (2,0,1,0), (0,0,1,2,2,0,0),
    (0,0,0,1,0,1,1), (0,0,0,2,1,0,2), (0,0,1,1,2,1,3), (1,3), (0,0,1,2,1,1,4), (0,1,0,1,0,0,0), (0,0,0,0,2,1,1),
    (0,1,1,1,3,0,3), (0,0,1,1,1,1,2), (1,4), (0,0,0,1,1,0,4), (0,0,0,2,1,1,0), (0,0,1,3,2,1,1), (0,0,0,2,3,1,3),
    (0,0,1,3,1,1,2), (0,0,0,2,2,1,4), (0,0,1,3,2,0,0), (0,0,1,2,3,0,2), (0,1,0,0,3,0,3), (1,5), (0,0,0,3,2,1,1),
    (0,0,0,3,3,1,4), (0,1,1,2,3,0,0), (0,1,1,0,3,0,1), (0,0,1,2,2,1,2), (0,0,1,2,0,1,3), (2,2,0,1), (2,2,1,1),
    (0,0,0,3,1,1,0), (0,0,0,1,3,1,1), (0,1,0,1,3,0,3), (0,1,1,1,3,1,4), (1,6), (0,0,1,3,3,0,2), (2,6,1,2),
    (0,0,1,2,3,1,4), (2,6,0,2), (0,1,0,2,0,0,0), (0,1,0,3,3,0,1), (0,0,1,3,3,1,3), (1,7), (0,1,1,2,0,0,2), (2,1,0,3),
    (0,1,1,2,3,1,4), (2,7,0,4), (0,1,1,3,3,0,1), (0,1,1,2,2,0,3), (0,1,1,1,0,1,2), (0,1,0,1,0,1,0), (2,4,0,5),
    (0,1,1,0,3,1,4), (2,3,0,6), (0,1,0,2,3,0,0), (0,1,0,3,0,1,1), (0,1,0,0,1,1,2), (0,1,0,0,3,1,3), (2,5,0,7),
    (0,1,1,3,0,1,1), (0,1,1,0,1,1,2), (0,1,0,1,2,0,3), (0,1,0,2,0,1,4), (3,0), (0,1,1,2,0,1,0), (4,0), (2,7,1,3),
    (0,1,0,3,2,0,3), (0,1,1,3,3,1,4), (2,1,1,4), (0,1,0,1,1,1,0), (0,1,0,3,3,1,1), (0,1,0,0,2,1,2), (3,2),
    (0,1,0,1,3,1,0), (0,1,0,3,1,1,1), (0,1,1,0,2,0,3), (0,1,0,2,3,1,4), (4,2), (0,1,0,2,1,1,2), (2,4,1,5), (3,1),
    (0,1,1,1,1,1,0), (0,1,1,3,1,1,1), (0,1,1,2,1,1,2), (0,1,1,2,2,1,3), (0,1,0,0,1,0,4), (4,1), (2,3,1,6),
    (0,1,0,3,2,1,4), (2,5,1,7), (0,1,1,1,2,0,0), (0,1,0,2,2,0,1), (0,1,1,0,1,0,3), (3,4), (0,1,0,2,2,1,2),
    (0,1,0,1,2,1,3), (0,1,1,0,2,1,4), (0,1,0,0,2,0,0), (0,1,1,3,2,0,1), (4,4), (5,0), (3,5), (0,1,1,3,2,1,0),
    (0,1,0,3,1,0,1), (0,1,1,1,2,1,3), (0,1,1,2,1,0,4), (6,0), (4,5), (5,2), (0,1,0,1,1,0,4), (0,1,0,2,1,0,3), (6,2),
    (5,1), (3,6), (6,1), (7,0), (4,6), (0,1,1,3,1,0,0), (0,1,1,1,1,0,1), (5,4), (3,7), (6,4), (7,2), (4,7), (5,5),
    (7,1), (7,4), (3,3), (6,5), (4,3), (5,6), (6,6), (5,7), (6,7), (5,3), (6,3), (7,5), (7,6), (7,7), (7,3),
)


def kernel(hidden, gain_in, up, up_scale_in, down, down_scale_in, out, gain, up_scale, down_scale, hbuf, ubuf, dbuf, other, w, x, acc, act, pbuf, sibp, own, zbuf, zrecv,
           in_sem, ag_send, ag_recv, tok_send, tok_recv, par_send, par_recv):
    rep, fs, core = lax.axis_index("rep"), lax.axis_index("fs"), lax.axis_index("tp")
    lo, yy, xx = fs // 16, (fs // 4) % 4, fs % 4
    turn = 1 + 2 * core

    def at(px, py, plo):
        return (plo * 4 + py) * 4 + px

    def neighbour(d):
        dx, dy, dz = STEP[d]
        return {"fs": at((xx + turn * dx) % 4, (yy + dy) % 4, (lo + dz) % 2)}

    sibling = {"tp": 1 - core}
    across = {"rep": 1 - rep, "fs": at(xx, yy, 1 - lo)}

    mine_q, far_q = (pl.ds(pl.multiple_of(r * Q, Q), Q) for r in (rep, 1 - rep))
    loads = [
        pltpu.make_async_copy(up.at[:, mine_q], ubuf.at[0], in_sem.at[0]),
        pltpu.make_async_copy(up.at[:, far_q], ubuf.at[1], in_sem.at[1]),
        pltpu.make_async_copy(down.at[:, mine_q], dbuf.at[0], in_sem.at[2]),
        pltpu.make_async_copy(hidden, hbuf, in_sem.at[3]),
        pltpu.make_async_copy(down.at[:, far_q], dbuf.at[1], in_sem.at[4]),
        pltpu.make_async_copy(gain_in, gain, in_sem.at[5]),
        pltpu.make_async_copy(up_scale_in.at[:, mine_q], up_scale, in_sem.at[6]),
        pltpu.make_async_copy(down_scale_in, down_scale, in_sem.at[7]),
    ]
    for load in loads:
        load.start()
    barrier = pltpu.get_barrier_semaphore()
    for peer in [neighbour(d) for d in range(5)] + [sibling, across]:
        pl.semaphore_signal(barrier, inc=1, device_id=peer, device_id_type=pl.DeviceIdType.MESH)

    me_rows = pl.ds(pl.multiple_of(fs * BLOCK, BLOCK), BLOCK)
    loads[0].wait()
    w[0, me_rows, :] = ubuf[0].astype(BF16)
    loads[1].wait()
    other[0] = ubuf[1].astype(BF16)
    loads[2].wait()
    w[1, me_rows, :] = dbuf[0].astype(BF16)
    pl.semaphore_wait(barrier, 7)

    def block_rows(o):
        return pl.ds(pl.multiple_of(at((xx + 4 - (turn * o[0]) % 4) % 4, (yy + 4 - o[1]) % 4, (lo + o[2]) % 2) * BLOCK, BLOCK), BLOCK)

    def remote(src, dst, send, recv, peer):
        return pltpu.make_async_remote_copy(src_ref=src, dst_ref=dst, send_sem=send, recv_sem=recv, device_id=peer,
                                            device_id_type=pl.DeviceIdType.MESH)

    def number(phase, half, o):
        return ((phase * CHUNKS + half) * 2 + o[2]) * 16 + o[1] * 4 + o[0]

    waited = set()

    def send_across(phase):
        for half in range(CHUNKS if phase else CHUNKS // 2):
            part = pl.ds(half * CHUNK, CHUNK)
            remote(other.at[phase, :, part], w.at[phase, me_rows, part], ag_send.at[phase],
                   ag_recv.at[number(phase, half, (0, 0, 1))], across).start()

    def block_copy(phase, half, o, d):
        s = STEP[d]
        held = ((o[0] - s[0]) % 4, (o[1] - s[1]) % 4, (o[2] - s[2]) % 2)
        ref = w.at[phase, block_rows(held), pl.ds(half * CHUNK, CHUNK)]
        return remote(ref, ref, ag_send.at[phase], ag_recv.at[number(phase, half, o)], neighbour(d))

    def need(phase, half, o):
        if o != (0, 0, 0) and (phase, half, o) not in waited:
            waited.add((phase, half, o))
            ref = w.at[phase, block_rows(o), pl.ds(half * CHUNK, CHUNK)]
            remote(ref, ref, ag_send.at[phase], ag_recv.at[number(phase, half, o)], sibling).wait_recv()

    def send(phase, half, o, d):
        s = STEP[d]
        held = ((o[0] - s[0]) % 4, (o[1] - s[1]) % 4, (o[2] - s[2]) % 2)
        need(phase, half, held)
        block_copy(phase, half, o, d).start()

    def need_group(phase, g):
        y, z = ORDER[phase][g]
        for half in range(CHUNKS):
            for a in range(4):
                need(phase, half, (a, y, z))

    def group(phase, g, far=0):
        y, z = ORDER[phase][g]
        return ((lo + far + z) % 2) * 4 + (yy + 4 - y) % 4

    def columns(a):
        return pl.ds(pl.multiple_of(a * GROUP, GROUP), GROUP)

    sib_far_rows, far_rows, sib_rows, my_rows = (pl.ds(i * ROWS, ROWS) for i in range(4))

    def token_far(g):
        a = group(0, g, 1)
        return remote(x.at[a, my_rows], x.at[a, far_rows], tok_send.at[0], tok_recv.at[0, g], across)

    def token_far_in(g):
        a = group(0, g)
        return remote(x.at[a, my_rows], x.at[a, far_rows], tok_send.at[0], tok_recv.at[0, g], across)

    def token_near(g):
        a = group(0, g)
        return remote(x.at[a, my_rows], x.at[a, sib_rows], tok_send.at[1], tok_recv.at[1, g], sibling)

    def token_relay(g):
        a = group(0, g)
        return remote(x.at[a, far_rows], x.at[a, sib_far_rows], tok_send.at[2], tok_recv.at[2, g], sibling)

    def near_part(g, i):
        return remote(pbuf.at[g, i], sibp.at[g, i], par_send.at[0], par_recv.at[i, g], sibling)

    def far_part(g):
        return remote(zbuf.at[g], zrecv.at[g], par_send.at[1], par_recv.at[2, g], across)

    plan = list(PLAN)
    while plan[0][0] == 0 and STEP[plan[0][6]] == tuple(plan[0][3:6]):
        send(plan[0][1], plan[0][2], plan[0][3:6], plan[0][6])
        plan.pop(0)
    send_across(0)
    loads[4].wait()
    other[1] = dbuf[1].astype(BF16)
    loads[3].wait()
    for load in loads[5:]:
        load.wait()

    @pl.loop(0, ROWS // 32)
    def _(i):
        rows = hbuf[pl.ds(i * 32, 32), :].astype(F32)
        inv = lax.rsqrt(jnp.mean(rows * rows, axis=1, keepdims=True) + 1e-06)
        normed = (rows * inv * gain[...]).astype(BF16)
        for a in range(8):
            x[a, pl.ds(3 * ROWS + i * 32, 32), :] = normed[:, a * GROUP:(a + 1) * GROUP]

    for g in range(8):
        token_far(g).start()
    send_across(1)
    for g in range(8):
        token_near(g).start()

    def up_product(g, part, n):
        need_group(0, g)
        if part == 0:
            token_relay(g).wait_recv()
        else:
            token_near(g).wait_recv()
        a, rows = group(0, g), pl.ds(part * 2 * ROWS, 2 * ROWS)

        @pl.loop(0, 2)
        def _(i):
            wide = pl.ds(pl.multiple_of(i * WIDE, WIDE), WIDE)
            total = jnp.dot(x[a, rows, :], w[0, columns(a), wide], preferred_element_type=F32)
            if n > 0:
                total = total + acc[i, rows, :]
            if n < 7:
                acc[i, rows, :] = total
            else:
                act[rows, wide] = jnp.square(jnp.maximum(total * up_scale[:, wide], 0.0)).astype(BF16)

    def mine(a):
        return acc.at[0, pl.ds(pl.multiple_of((a % 4) * ROWS, ROWS), ROWS), columns(a // 4)]

    def products(first, a, g):
        @pl.loop(0, 2)
        def _(i):
            rows = pl.ds(pl.multiple_of((2 * first + i) * ROWS, ROWS), ROWS)
            part = lax.dot_general(act[rows, :], w[1, columns(a), :], (((1,), (1,)), ((), ())), preferred_element_type=F32)
            own[first, i] = part

            @pl.when(i == 0)
            def _():
                pbuf[g, first] = part.astype(BF16)
                near_part(g, first).start()

    def down_far(g):
        need_group(1, g)
        products(0, group(1, g), g)

    def sum_far(g):
        near_part(g, 0).wait_recv()
        zbuf[g] = (own[0, 1] + sibp[g, 0].astype(F32)).astype(BF16)
        far_part(g).start()

    def down_near(g):
        products(1, group(1, g), g)

    def output_sum(g):
        near_part(g, 1).wait_recv()
        mine(group(1, g))[...] = own[1, 1] + sibp[g, 1].astype(F32)

    def output(g):
        a = group(1, g, 1)
        far_part(g).wait_recv()
        out[:, columns(a)] = ((mine(a)[...] + zrecv[g].astype(F32)) * down_scale[:, columns(a)]).astype(BF16)

    for step in plan:
        kind, arg = step[0], step[1]
        if kind == 0:
            send(arg, step[2], step[3:6], step[6])
        elif kind == 1:
            token_far_in(arg).wait_recv()
            token_relay(arg).start()
        elif kind == 2:
            up_product(arg, step[2], step[3])
        elif kind == 3:
            down_far(arg)
        elif kind == 4:
            sum_far(arg)
        elif kind == 5:
            down_near(arg)
        elif kind == 6:
            output_sum(arg)
        else:
            output(arg)

    for phase in range(2):
        sent = w.at[phase, pl.ds(0, 31 * BLOCK), :]
        remote(sent, sent, ag_send.at[phase], ag_recv.at[0], sibling).wait_send()
    for i in range(3):
        sent = x.at[:, pl.ds(0, ROWS)]
        remote(sent, sent, tok_send.at[i], tok_recv.at[0, 0], sibling).wait_send()
    remote(sibp, sibp, par_send.at[0], par_recv.at[0, 0], sibling).wait_send()
    remote(zbuf, zbuf, par_send.at[1], par_recv.at[0, 0], sibling).wait_send()


def body(hidden_in, norm_gain, up_weight, up_scale, down_weight, down_scale):
    vmem, anywhere = pl.BlockSpec(memory_space=pltpu.VMEM), pl.BlockSpec(memory_space=pl.ANY)
    dma = pltpu.SemaphoreType.DMA
    return pl.pallas_call(
        kernel,
        out_shape=pltpu.VMEM((ROWS, D), BF16),
        in_specs=[anywhere] * 6,
        out_specs=vmem,
        scratch_shapes=[
            pltpu.VMEM((1, D), F32),
            pltpu.VMEM((1, Q), F32),
            pltpu.VMEM((1, D), F32),
            pltpu.VMEM((ROWS, D), BF16),
            pltpu.VMEM((2, BLOCK, Q), F32),
            pltpu.VMEM((2, BLOCK, Q), F32),
            pltpu.VMEM((2, BLOCK, Q), BF16),
            pltpu.VMEM((2, D, Q), BF16),
            pltpu.VMEM((8, 4 * ROWS, GROUP), BF16),
            pltpu.VMEM((Q // WIDE, 4 * ROWS, WIDE), F32),
            pltpu.VMEM((4 * ROWS, Q), BF16),
            pltpu.VMEM((8, 2, ROWS, GROUP), BF16),
            pltpu.VMEM((8, 2, ROWS, GROUP), BF16),
            pltpu.VMEM((2, 2, ROWS, GROUP), F32),
            pltpu.VMEM((8, ROWS, GROUP), BF16),
            pltpu.VMEM((8, ROWS, GROUP), BF16),
            dma((8,)),
            dma((2,)),
            dma((CHUNKS * 64,)),
            dma((3,)),
            dma((3, 8)),
            dma((2,)),
            dma((3, 8)),
        ],
        compiler_params=pltpu.CompilerParams(collective_id=0, has_side_effects=True, vmem_limit_bytes=63000000),
        name="ffn",
    )(hidden_in, norm_gain.reshape(1, -1), up_weight, up_scale.reshape(1, -1), down_weight.T, down_scale.reshape(1, -1))


def solution(mesh):
    placed = (P(("rep", "fs", "tp"), None), P(), P("fs", "tp"), P("tp"), P("tp", "fs"), P())
    return jax.shard_map(
        body, mesh=mesh, in_specs=placed, out_specs=P(("rep", "fs", "tp"), None), check_vma=False
    )
```

```python
import jax
import jax.numpy as jnp
from jax import lax
from jax.experimental import pallas as pl
from jax.experimental.pallas import tpu as pltpu
from jax.sharding import PartitionSpec as P

F32, BF16 = jnp.float32, jnp.bfloat16
ROWS, D, Q, GROUP, BLOCK = 384, 2048, 2048, 256, 64
CHUNKS, WIDE = 2, Q // 2
CHUNK = Q // CHUNKS
STEP = ((1, 0, 0), (3, 0, 0), (0, 1, 0), (0, 3, 0), (0, 0, 1))
ORDER = (
    ((0, 0), (0, 1), (1, 0), (3, 0), (1, 1), (3, 1), (2, 0), (2, 1)),
    ((0, 0), (0, 1), (3, 0), (1, 0), (3, 1), (1, 1), (2, 0), (2, 1)),
)
PLAN = (
    (0,0,0,1,0,0,0), (0,0,0,3,0,0,1), (0,0,0,0,1,0,2), (0,0,1,0,3,0,3), (0,0,1,0,0,1,4), (0,0,1,1,0,0,0),
    (0,1,0,3,0,0,1), (0,0,1,0,1,0,2), (0,1,1,0,3,0,3), (0,0,0,3,0,1,4), (0,0,1,1,0,1,0), (0,0,1,3,3,0,1),
    (0,0,0,0,2,0,2), (0,0,1,0,2,0,3), (0,0,1,0,3,1,4), (0,0,1,2,0,0,0), (0,0,0,2,0,0,1), (0,0,0,1,1,0,2),
    (0,0,1,1,3,0,3), (1,0), (0,0,0,0,2,1,4), (0,0,1,2,0,1,0), (0,0,1,2,3,0,1), (0,0,1,1,1,1,2), (0,0,0,3,3,0,3),
    (0,0,1,0,2,1,4), (1,1), (0,0,1,3,0,0,0), (0,0,1,3,0,1,1), (0,0,0,1,2,0,2), (0,0,0,2,3,0,3), (0,0,1,1,3,1,0),
    (0,0,0,2,0,1,1), (0,0,0,0,1,1,2), (0,0,1,3,2,0,3), (0,0,1,1,1,0,4), (0,0,0,3,3,1,4), (1,2), (0,0,0,2,1,0,0),
    (0,0,0,3,2,1,1), (0,0,1,2,1,1,2), (0,0,1,2,2,0,3), (2,0,0,0), (0,0,0,2,3,1,4), (2,0,1,0), (0,1,1,1,0,0,0),
    (0,1,1,3,3,0,1), (0,0,1,3,1,0,2), (0,0,1,3,3,1,3), (1,3), (0,0,0,1,2,1,4), (0,0,0,1,1,1,0), (0,0,0,1,0,1,1),
    (0,0,0,1,3,0,2), (0,0,1,1,2,0,3), (0,0,0,3,2,0,4), (1,4), (0,0,0,3,1,0,0), (0,1,1,3,0,0,1), (0,0,1,3,1,1,2),
    (0,0,1,2,1,0,3), (0,0,1,2,2,1,4), (0,1,0,1,0,0,0), (0,1,1,2,3,0,1), (0,0,0,2,2,0,2), (0,0,0,3,1,1,3), (1,5),
    (2,1,0,1), (0,0,0,2,1,1,4), (2,1,1,1), (0,0,0,0,3,0,1), (0,0,1,1,2,1,2), (0,1,0,3,3,0,3), (0,0,1,0,1,1,0),
    (2,2,0,2), (0,0,0,1,3,1,4), (1,6), (2,2,1,2), (0,0,1,3,2,1,0), (0,1,1,2,0,0,1), (0,0,1,2,3,1,2), (0,0,0,0,3,1,3),
    (2,6,0,3), (0,0,0,2,2,1,4), (2,6,1,3), (0,1,0,2,0,0,0), (0,1,1,1,3,0,1), (0,1,0,1,1,0,2), (0,1,0,1,3,0,3), (1,7),
    (2,4,0,4), (0,1,1,3,0,1,4), (2,3,0,5), (0,1,0,0,3,0,0), (0,1,0,2,3,0,1), (0,1,1,0,1,0,2), (0,1,0,3,2,0,3),
    (2,5,0,6), (0,1,1,2,0,1,4), (0,1,0,1,0,1,0), (0,1,0,3,0,1,1), (0,1,1,2,1,0,2), (0,1,0,0,3,1,3), (2,7,0,7), (3,0),
    (0,1,1,1,0,1,0), (0,1,0,0,1,0,1), (0,1,0,2,1,0,2), (0,1,1,0,3,1,3), (0,1,0,2,0,1,4), (4,0), (3,2),
    (0,1,1,1,1,0,0), (0,1,1,3,1,0,1), (0,1,1,0,2,0,2), (0,1,0,3,1,0,3), (0,1,0,2,3,1,4), (4,2), (2,4,1,4), (2,3,1,5),
    (0,1,0,1,3,1,0), (0,1,0,3,3,1,1), (0,1,0,1,2,0,2), (0,1,1,2,3,1,3), (0,1,0,1,1,1,4), (2,5,1,6), (3,1),
    (0,1,1,1,3,1,0), (0,1,1,3,3,1,1), (0,1,0,2,2,0,2), (0,1,0,0,2,0,3), (0,1,0,3,2,1,4), (4,1), (2,7,1,7), (3,3),
    (0,1,1,1,2,0,0), (0,1,1,3,2,0,1), (0,1,1,2,2,0,2), (0,1,1,0,2,1,3), (0,1,1,1,1,1,4), (4,3), (5,0),
    (0,1,0,2,1,1,0), (0,1,0,0,1,1,1), (0,1,0,3,1,1,2), (0,1,1,2,2,1,3), (0,1,0,1,2,1,4), (6,0), (5,2), (3,4),
    (0,1,1,3,1,1,2), (0,1,1,1,2,1,3), (0,1,0,0,2,1,4), (6,2), (0,1,1,2,1,1,0), (0,1,1,0,1,1,1), (4,4), (3,6),
    (0,1,0,2,2,1,4), (4,6), (5,1), (0,1,1,3,2,1,0), (6,1), (5,3), (7,0), (3,5), (6,3), (4,5), (5,4), (3,7), (6,4),
    (7,2), (4,7), (5,6), (7,1), (6,6), (5,5), (6,5), (5,7), (7,3), (7,4), (6,7), (7,6), (7,5), (7,7),
)


def kernel(hidden, gain_in, up, up_scale_in, down, down_scale_in, out, gain, up_scale, down_scale, hbuf, ubuf, dbuf, other, w, x, acc, act, pbuf, sibp, own, zbuf, zrecv,
           in_sem, ag_send, ag_recv, tok_send, tok_recv, par_send, par_recv):
    rep, fs, core = lax.axis_index("rep"), lax.axis_index("fs"), lax.axis_index("tp")
    lo, yy, xx = fs // 16, (fs // 4) % 4, fs % 4
    turn = 1 + 2 * core

    def at(px, py, plo):
        return (plo * 4 + py) * 4 + px

    def neighbour(d):
        dx, dy, dz = STEP[d]
        return {"fs": at((xx + turn * dx) % 4, (yy + dy) % 4, (lo + dz) % 2)}

    sibling = {"tp": 1 - core}
    across = {"rep": 1 - rep, "fs": at(xx, yy, 1 - lo)}

    mine_q, far_q = (pl.ds(pl.multiple_of(r * Q, Q), Q) for r in (rep, 1 - rep))
    loads = [
        pltpu.make_async_copy(up.at[:, mine_q], ubuf.at[0], in_sem.at[0]),
        pltpu.make_async_copy(up.at[:, far_q], ubuf.at[1], in_sem.at[1]),
        pltpu.make_async_copy(down.at[:, mine_q], dbuf.at[0], in_sem.at[2]),
        pltpu.make_async_copy(hidden, hbuf, in_sem.at[3]),
        pltpu.make_async_copy(down.at[:, far_q], dbuf.at[1], in_sem.at[4]),
        pltpu.make_async_copy(gain_in, gain, in_sem.at[5]),
        pltpu.make_async_copy(up_scale_in.at[:, mine_q], up_scale, in_sem.at[6]),
        pltpu.make_async_copy(down_scale_in, down_scale, in_sem.at[7]),
    ]
    for load in loads:
        load.start()
    barrier = pltpu.get_barrier_semaphore()
    for peer in [neighbour(d) for d in range(5)] + [sibling, across]:
        pl.semaphore_signal(barrier, inc=1, device_id=peer, device_id_type=pl.DeviceIdType.MESH)

    me_rows = pl.ds(pl.multiple_of(fs * BLOCK, BLOCK), BLOCK)
    loads[0].wait()
    w[0, me_rows, :] = ubuf[0].astype(BF16)
    pl.semaphore_wait(barrier, 7)

    def block_rows(o):
        return pl.ds(pl.multiple_of(at((xx + 4 - (turn * o[0]) % 4) % 4, (yy + 4 - o[1]) % 4, (lo + o[2]) % 2) * BLOCK, BLOCK), BLOCK)

    def remote(src, dst, send, recv, peer):
        return pltpu.make_async_remote_copy(src_ref=src, dst_ref=dst, send_sem=send, recv_sem=recv, device_id=peer,
                                            device_id_type=pl.DeviceIdType.MESH)

    def number(phase, half, o):
        return ((phase * CHUNKS + half) * 2 + o[2]) * 16 + o[1] * 4 + o[0]

    waited = set()

    def send_across(phase):
        for half in range(CHUNKS if phase else CHUNKS // 2):
            part = pl.ds(half * CHUNK, CHUNK)
            remote(other.at[phase, :, part], w.at[phase, me_rows, part], ag_send.at[phase],
                   ag_recv.at[number(phase, half, (0, 0, 1))], across).start()

    def block_copy(phase, half, o, d):
        s = STEP[d]
        held = ((o[0] - s[0]) % 4, (o[1] - s[1]) % 4, (o[2] - s[2]) % 2)
        ref = w.at[phase, block_rows(held), pl.ds(half * CHUNK, CHUNK)]
        return remote(ref, ref, ag_send.at[phase], ag_recv.at[number(phase, half, o)], neighbour(d))

    def need(phase, half, o):
        if o != (0, 0, 0) and (phase, half, o) not in waited:
            waited.add((phase, half, o))
            ref = w.at[phase, block_rows(o), pl.ds(half * CHUNK, CHUNK)]
            remote(ref, ref, ag_send.at[phase], ag_recv.at[number(phase, half, o)], sibling).wait_recv()

    def send(phase, half, o, d):
        s = STEP[d]
        held = ((o[0] - s[0]) % 4, (o[1] - s[1]) % 4, (o[2] - s[2]) % 2)
        need(phase, half, held)
        block_copy(phase, half, o, d).start()

    def need_group(phase, g):
        y, z = ORDER[phase][g]
        for half in range(CHUNKS):
            for a in range(4):
                need(phase, half, (a, y, z))

    def group(phase, g, far=0):
        y, z = ORDER[phase][g]
        return ((lo + far + z) % 2) * 4 + (yy + 4 - y) % 4

    def columns(a):
        return pl.ds(pl.multiple_of(a * GROUP, GROUP), GROUP)

    sib_far_rows, far_rows, sib_rows, my_rows = (pl.ds(i * ROWS, ROWS) for i in range(4))

    def token_far(g):
        a = group(0, g, 1)
        return remote(x.at[a, my_rows], x.at[a, far_rows], tok_send.at[0], tok_recv.at[0, g], across)

    def token_far_in(g):
        a = group(0, g)
        return remote(x.at[a, my_rows], x.at[a, far_rows], tok_send.at[0], tok_recv.at[0, g], across)

    def token_near(g):
        a = group(0, g)
        return remote(x.at[a, my_rows], x.at[a, sib_rows], tok_send.at[1], tok_recv.at[1, g], sibling)

    def token_relay(g):
        a = group(0, g)
        return remote(x.at[a, far_rows], x.at[a, sib_far_rows], tok_send.at[2], tok_recv.at[2, g], sibling)

    def near_part(g, i):
        return remote(pbuf.at[g, i], sibp.at[g, i], par_send.at[0], par_recv.at[i, g], sibling)

    def far_part(g):
        return remote(zbuf.at[g], zrecv.at[g], par_send.at[1], par_recv.at[2, g], across)

    plan = list(PLAN)
    while plan[0][:2] == (0, 0) and STEP[plan[0][6]] == tuple(plan[0][3:6]):
        send(plan[0][1], plan[0][2], plan[0][3:6], plan[0][6])
        plan.pop(0)
    loads[1].wait()
    other[0] = ubuf[1].astype(BF16)
    send_across(0)
    for i, to in ((2, w.at[1, me_rows]), (4, other.at[1])):
        loads[i].wait()
        to[...] = dbuf[i // 4].astype(BF16)
    loads[3].wait()
    for load in loads[5:]:
        load.wait()

    @pl.loop(0, ROWS // 32)
    def _(i):
        rows = hbuf[pl.ds(i * 32, 32), :].astype(F32)
        inv = lax.rsqrt(jnp.mean(rows * rows, axis=1, keepdims=True) + 1e-06)
        normed = (rows * inv * gain[...]).astype(BF16)
        for a in range(8):
            x[a, pl.ds(3 * ROWS + i * 32, 32), :] = normed[:, a * GROUP:(a + 1) * GROUP]

    for g in range(8):
        token_far(g).start()
    send_across(1)
    for g in range(8):
        token_near(g).start()

    def up_product(g, part, n):
        need_group(0, g)
        if part == 0:
            token_relay(g).wait_recv()
        else:
            token_near(g).wait_recv()
        a, rows = group(0, g), pl.ds(part * 2 * ROWS, 2 * ROWS)

        @pl.loop(0, 2)
        def _(i):
            wide = pl.ds(pl.multiple_of(i * WIDE, WIDE), WIDE)
            total = jnp.dot(x[a, rows, :], w[0, columns(a), wide], preferred_element_type=F32)
            if n > 0:
                total = total + acc[i, rows, :]
            if n < 7:
                acc[i, rows, :] = total
            else:
                act[rows, wide] = jnp.square(jnp.maximum(total * up_scale[:, wide], 0.0)).astype(BF16)

    def mine(a):
        return acc.at[0, pl.ds(pl.multiple_of((a % 4) * ROWS, ROWS), ROWS), columns(a // 4)]

    def products(first, a, g):
        @pl.loop(0, 2)
        def _(i):
            rows = pl.ds(pl.multiple_of((2 * first + i) * ROWS, ROWS), ROWS)
            part = lax.dot_general(act[rows, :], w[1, columns(a), :], (((1,), (1,)), ((), ())), preferred_element_type=F32)
            own[first, i] = part

            @pl.when(i == 0)
            def _():
                pbuf[g, first] = part.astype(BF16)
                near_part(g, first).start()

    def down_far(g):
        need_group(1, g)
        products(0, group(1, g), g)

    def sum_far(g):
        near_part(g, 0).wait_recv()
        zbuf[g] = (own[0, 1] + sibp[g, 0].astype(F32)).astype(BF16)
        far_part(g).start()

    def down_near(g):
        products(1, group(1, g), g)

    def output_sum(g):
        near_part(g, 1).wait_recv()
        mine(group(1, g))[...] = own[1, 1] + sibp[g, 1].astype(F32)

    def output(g):
        a = group(1, g, 1)
        far_part(g).wait_recv()
        out[:, columns(a)] = ((mine(a)[...] + zrecv[g].astype(F32)) * down_scale[:, columns(a)]).astype(BF16)

    for step in plan:
        kind, arg = step[0], step[1]
        if kind == 0:
            send(arg, step[2], step[3:6], step[6])
        elif kind == 1:
            token_far_in(arg).wait_recv()
            token_relay(arg).start()
        elif kind == 2:
            up_product(arg, step[2], step[3])
        elif kind == 3:
            down_far(arg)
        elif kind == 4:
            sum_far(arg)
        elif kind == 5:
            down_near(arg)
        elif kind == 6:
            output_sum(arg)
        else:
            output(arg)

    for phase in range(2):
        sent = w.at[phase, pl.ds(0, 31 * BLOCK), :]
        remote(sent, sent, ag_send.at[phase], ag_recv.at[0], sibling).wait_send()
    for i in range(3):
        sent = x.at[:, pl.ds(0, ROWS)]
        remote(sent, sent, tok_send.at[i], tok_recv.at[0, 0], sibling).wait_send()
    remote(sibp, sibp, par_send.at[0], par_recv.at[0, 0], sibling).wait_send()
    remote(zbuf, zbuf, par_send.at[1], par_recv.at[0, 0], sibling).wait_send()


def body(hidden_in, norm_gain, up_weight, up_scale, down_weight, down_scale):
    vmem, anywhere = pl.BlockSpec(memory_space=pltpu.VMEM), pl.BlockSpec(memory_space=pl.ANY)
    dma = pltpu.SemaphoreType.DMA
    return pl.pallas_call(
        kernel,
        out_shape=pltpu.VMEM((ROWS, D), BF16),
        in_specs=[anywhere] * 6,
        out_specs=vmem,
        scratch_shapes=[
            pltpu.VMEM((1, D), F32),
            pltpu.VMEM((1, Q), F32),
            pltpu.VMEM((1, D), F32),
            pltpu.VMEM((ROWS, D), BF16),
            pltpu.VMEM((2, BLOCK, Q), F32),
            pltpu.VMEM((2, BLOCK, Q), F32),
            pltpu.VMEM((2, BLOCK, Q), BF16),
            pltpu.VMEM((2, D, Q), BF16),
            pltpu.VMEM((8, 4 * ROWS, GROUP), BF16),
            pltpu.VMEM((Q // WIDE, 4 * ROWS, WIDE), F32),
            pltpu.VMEM((4 * ROWS, Q), BF16),
            pltpu.VMEM((8, 2, ROWS, GROUP), BF16),
            pltpu.VMEM((8, 2, ROWS, GROUP), BF16),
            pltpu.VMEM((2, 2, ROWS, GROUP), F32),
            pltpu.VMEM((8, ROWS, GROUP), BF16),
            pltpu.VMEM((8, ROWS, GROUP), BF16),
            dma((8,)),
            dma((2,)),
            dma((CHUNKS * 64,)),
            dma((3,)),
            dma((3, 8)),
            dma((2,)),
            dma((3, 8)),
        ],
        compiler_params=pltpu.CompilerParams(collective_id=0, has_side_effects=True, vmem_limit_bytes=63000000),
        name="ffn",
    )(hidden_in, norm_gain.reshape(1, -1), up_weight, up_scale.reshape(1, -1), down_weight.T, down_scale.reshape(1, -1))


def solution(mesh):
    placed = (P(("rep", "fs", "tp"), None), P(), P("fs", "tp"), P("tp"), P("tp", "fs"), P())
    return jax.shard_map(
        body, mesh=mesh, in_specs=placed, out_specs=P(("rep", "fs", "tp"), None), check_vma=False
    )
```

```python
import jax
import jax.numpy as jnp
from jax import lax
from jax.experimental import pallas as pl
from jax.experimental.pallas import tpu as pltpu
from jax.sharding import PartitionSpec as P

F32, BF16 = jnp.float32, jnp.bfloat16
ROWS, D, Q, GROUP, BLOCK = 384, 2048, 2048, 256, 64
CHUNKS, WIDE = 2, Q // 2
CHUNK = Q // CHUNKS
STEP = ((1, 0, 0), (3, 0, 0), (0, 1, 0), (0, 3, 0), (0, 0, 1))
ORDER = (
    ((0, 0), (0, 1), (1, 0), (3, 0), (1, 1), (3, 1), (2, 0), (2, 1)),
    ((0, 0), (0, 1), (3, 0), (1, 0), (3, 1), (1, 1), (2, 0), (2, 1)),
)
PLAN = (
    (0,0,0,1,0,0,0), (0,0,1,3,0,0,1), (0,0,0,0,1,0,2), (0,0,0,0,3,0,3), (0,0,1,0,0,1,4), (0,1,0,1,0,0,0),
    (0,1,0,3,0,0,1), (0,0,1,0,1,0,2), (0,1,0,0,3,0,3), (0,0,0,1,0,1,4), (0,0,1,1,0,1,0), (0,0,0,3,3,0,1),
    (0,0,0,1,1,0,2), (0,0,1,3,3,0,3), (0,0,0,0,1,1,4), (0,1,0,1,3,0,0), (0,0,1,2,0,0,1), (0,0,1,0,2,0,2),
    (0,0,0,0,3,1,3), (1,0), (0,0,0,3,3,1,4), (0,0,1,1,0,0,0), (0,0,0,3,0,1,1), (0,0,1,1,1,1,2), (0,0,0,3,2,0,3),
    (0,0,0,1,1,1,4), (1,1), (0,0,0,1,3,1,0), (0,0,1,3,0,1,1), (0,0,1,2,1,0,2), (0,0,1,2,3,0,3), (0,0,1,0,2,1,4),
    (0,1,1,1,0,0,0), (0,1,0,2,0,0,1), (0,0,1,0,1,1,2), (0,0,1,3,2,0,3), (2,0,0,0,1), (2,0,1,0,1), (0,0,0,3,0,0,4),
    (1,2), (0,0,0,2,0,1,0), (0,0,0,2,2,0,1), (0,0,0,0,2,1,2), (0,0,0,3,1,0,3), (0,0,1,2,1,1,4), (0,0,0,2,3,1,0),
    (0,0,1,1,1,0,1), (0,0,0,1,2,1,2), (0,0,1,2,2,0,3), (1,3), (0,0,0,1,3,0,4), (0,0,1,1,2,1,0), (0,0,1,1,3,0,1),
    (0,0,1,3,1,0,2), (0,1,0,2,3,0,3), (2,1,0,0,0), (2,1,1,0,0), (0,0,0,3,1,1,4), (1,4), (0,0,1,2,0,1,0),
    (0,0,0,2,1,0,1), (0,1,0,1,1,0,2), (0,0,1,3,3,1,3), (2,5,1,1,0), (0,0,0,2,3,0,4), (0,0,1,3,1,1,0),
    (0,0,1,3,2,1,1), (0,0,1,2,2,1,2), (0,0,0,2,2,1,3), (1,5), (2,2,0,1,1), (2,2,1,1,1), (0,0,0,0,2,0,4), (2,5,0,1,0),
    (0,1,1,2,0,0,0), (0,0,1,0,3,0,1), (0,0,1,1,3,1,2), (0,0,1,1,2,0,3), (2,1,0,2,1), (2,2,0,2,0), (0,0,0,1,2,0,4),
    (1,6), (2,1,1,2,1), (0,0,1,0,3,1,0), (0,0,1,2,3,1,1), (0,0,0,3,2,1,2), (0,0,0,2,0,0,3), (2,3,0,3,0), (2,4,0,3,1),
    (2,2,1,2,0), (0,1,0,3,3,0,1), (0,1,1,0,1,0,2), (0,1,1,1,3,0,3), (0,0,0,2,1,1,4), (2,3,1,3,0), (2,4,1,3,1),
    (0,1,1,3,0,0,0), (1,7), (2,3,0,4,1), (2,6,0,5,1), (0,1,1,2,0,1,4), (0,1,1,2,1,0,2), (0,1,1,0,3,0,3), (2,7,0,6,1),
    (2,6,0,4,0), (0,1,0,1,0,1,0), (0,1,0,3,0,1,1), (2,5,0,7,1), (2,7,0,5,0), (0,1,0,3,1,0,2), (0,1,0,1,3,1,4),
    (2,0,0,6,0), (2,4,0,7,0), (0,1,1,2,3,0,0), (0,1,1,3,0,1,1), (0,1,1,3,3,0,3), (3,0), (0,1,1,3,1,0,2),
    (0,1,1,0,1,1,4), (4,0), (0,1,1,1,0,1,1), (0,1,1,2,3,1,3), (2,7,1,4,1), (0,1,0,2,0,1,0), (2,3,1,5,1),
    (0,1,1,0,3,1,4), (2,6,1,6,1), (0,1,1,1,1,0,1), (0,1,0,1,1,1,2), (0,1,0,3,3,1,3), (2,6,1,4,0), (0,1,0,0,1,0,0),
    (3,2), (0,1,0,3,1,1,4), (0,1,1,0,2,0,2), (0,1,0,2,1,0,1), (4,2), (2,5,1,7,1), (0,1,1,1,1,1,0), (0,1,1,2,2,1,3),
    (3,1), (0,1,1,3,3,1,4), (0,1,1,3,1,1,2), (0,1,1,1,3,1,1), (0,1,0,2,3,1,3), (4,1), (2,7,1,5,0), (2,0,1,6,0),
    (0,1,0,0,3,1,0), (2,4,1,7,0), (0,1,0,0,1,1,4), (5,0), (0,1,0,2,1,1,1), (0,1,0,1,2,1,2), (0,1,0,3,2,1,3),
    (0,1,1,2,1,1,0), (3,3), (0,1,1,0,2,1,4), (6,0), (0,1,1,3,2,0,1), (0,1,0,2,2,0,2), (4,3), (0,1,1,3,2,1,0), (5,2),
    (0,1,1,1,2,1,3), (3,4), (0,1,0,0,2,0,2), (0,1,1,2,2,0,4), (6,2), (4,4), (5,1), (0,1,0,0,2,1,0), (0,1,0,2,2,1,1),
    (3,5), (6,1), (7,0), (0,1,0,3,2,0,0), (0,1,0,1,2,0,1), (0,1,1,1,2,0,4), (4,5), (5,3), (6,3), (5,4), (3,7), (6,4),
    (7,2), (4,7), (5,5), (3,6), (6,5), (7,1), (4,6), (5,7), (7,3), (7,4), (6,7), (5,6), (7,5), (6,6), (7,7), (7,6),
)


def kernel(hidden, gain_in, up, up_scale_in, down, down_scale_in, out, gain, up_scale, down_scale, hbuf, ubuf, dbuf, other, w, x, acc, act, pbuf, sibp, own, zbuf, zrecv,
           in_sem, ag_send, ag_recv, tok_send, tok_recv, par_send, par_recv):
    rep, fs, core = lax.axis_index("rep"), lax.axis_index("fs"), lax.axis_index("tp")
    lo, yy, xx = fs // 16, (fs // 4) % 4, fs % 4
    turn = 1 + 2 * core

    def at(px, py, plo):
        return (plo * 4 + py) * 4 + px

    def neighbour(d):
        dx, dy, dz = STEP[d]
        return {"fs": at((xx + turn * dx) % 4, (yy + dy) % 4, (lo + dz) % 2)}

    sibling = {"tp": 1 - core}
    across = {"rep": 1 - rep, "fs": at(xx, yy, 1 - lo)}

    mine_q, far_q = (pl.ds(pl.multiple_of(r * Q, Q), Q) for r in (rep, 1 - rep))
    loads = [
        pltpu.make_async_copy(up.at[:, mine_q], ubuf.at[0], in_sem.at[0]),
        pltpu.make_async_copy(up.at[:, far_q], ubuf.at[1], in_sem.at[1]),
        pltpu.make_async_copy(down.at[:, mine_q], dbuf.at[0], in_sem.at[2]),
        pltpu.make_async_copy(hidden, hbuf, in_sem.at[3]),
        pltpu.make_async_copy(down.at[:, far_q], dbuf.at[1], in_sem.at[4]),
        pltpu.make_async_copy(gain_in, gain, in_sem.at[5]),
        pltpu.make_async_copy(up_scale_in.at[:, mine_q], up_scale, in_sem.at[6]),
        pltpu.make_async_copy(down_scale_in, down_scale, in_sem.at[7]),
    ]
    for load in loads:
        load.start()
    barrier = pltpu.get_barrier_semaphore()
    for peer in [neighbour(d) for d in range(5)] + [sibling, across]:
        pl.semaphore_signal(barrier, inc=1, device_id=peer, device_id_type=pl.DeviceIdType.MESH)

    me_rows = pl.ds(pl.multiple_of(fs * BLOCK, BLOCK), BLOCK)
    loads[0].wait()
    w[0, me_rows, :] = ubuf[0].astype(BF16)
    pl.semaphore_wait(barrier, 7)

    def block_rows(o):
        return pl.ds(pl.multiple_of(at((xx + 4 - (turn * o[0]) % 4) % 4, (yy + 4 - o[1]) % 4, (lo + o[2]) % 2) * BLOCK, BLOCK), BLOCK)

    def remote(src, dst, send, recv, peer):
        return pltpu.make_async_remote_copy(src_ref=src, dst_ref=dst, send_sem=send, recv_sem=recv, device_id=peer,
                                            device_id_type=pl.DeviceIdType.MESH)

    def number(phase, half, o):
        return ((phase * CHUNKS + half) * 2 + o[2]) * 16 + o[1] * 4 + o[0]

    waited, fed = set(), set()

    def send_across(phase):
        for half in range(CHUNKS if phase else CHUNKS // 2):
            part = pl.ds(half * CHUNK, CHUNK)
            remote(other.at[phase, :, part], w.at[phase, me_rows, part], ag_send.at[phase],
                   ag_recv.at[number(phase, half, (0, 0, 1))], across).start()

    def block_copy(phase, half, o, d):
        s = STEP[d]
        held = ((o[0] - s[0]) % 4, (o[1] - s[1]) % 4, (o[2] - s[2]) % 2)
        ref = w.at[phase, block_rows(held), pl.ds(half * CHUNK, CHUNK)]
        return remote(ref, ref, ag_send.at[phase], ag_recv.at[number(phase, half, o)], neighbour(d))

    def need(phase, half, o):
        if o != (0, 0, 0) and (phase, half, o) not in waited:
            waited.add((phase, half, o))
            ref = w.at[phase, block_rows(o), pl.ds(half * CHUNK, CHUNK)]
            remote(ref, ref, ag_send.at[phase], ag_recv.at[number(phase, half, o)], sibling).wait_recv()

    def send(phase, half, o, d):
        s = STEP[d]
        held = ((o[0] - s[0]) % 4, (o[1] - s[1]) % 4, (o[2] - s[2]) % 2)
        need(phase, half, held)
        block_copy(phase, half, o, d).start()

    def need_group(phase, g):
        y, z = ORDER[phase][g]
        for half in range(CHUNKS):
            for a in range(4):
                need(phase, half, (a, y, z))

    def group(phase, g, far=0):
        y, z = ORDER[phase][g]
        return ((lo + far + z) % 2) * 4 + (yy + 4 - y) % 4

    def columns(a):
        return pl.ds(pl.multiple_of(a * GROUP, GROUP), GROUP)

    sib_far_rows, far_rows, sib_rows, my_rows = (pl.ds(i * ROWS, ROWS) for i in range(4))

    def token_far(g):
        a = group(0, g, 1)
        return remote(x.at[a, my_rows], x.at[a, far_rows], tok_send.at[0], tok_recv.at[0, g], across)

    def token_far_in(g):
        a = group(0, g)
        return remote(x.at[a, my_rows], x.at[a, far_rows], tok_send.at[0], tok_recv.at[0, g], across)

    def token_near(g):
        a = group(0, g)
        return remote(x.at[a, my_rows], x.at[a, sib_rows], tok_send.at[1], tok_recv.at[1, g], sibling)

    def token_relay(g):
        a = group(0, g)
        return remote(x.at[a, far_rows], x.at[a, sib_far_rows], tok_send.at[2], tok_recv.at[2, g], sibling)

    def near_part(g, i):
        return remote(pbuf.at[g, i], sibp.at[g, i], par_send.at[0], par_recv.at[i, g], sibling)

    def far_part(g):
        return remote(zbuf.at[g], zrecv.at[g], par_send.at[1], par_recv.at[2, g], across)

    plan = list(PLAN)
    while plan[0][:2] == (0, 0) and STEP[plan[0][6]] == tuple(plan[0][3:6]):
        send(plan[0][1], plan[0][2], plan[0][3:6], plan[0][6])
        plan.pop(0)
    loads[1].wait()
    other[0] = ubuf[1].astype(BF16)
    send_across(0)
    for i, to in ((2, w.at[1, me_rows]), (4, other.at[1])):
        loads[i].wait()
        to[...] = dbuf[i // 4].astype(BF16)
    loads[3].wait()
    for load in loads[5:]:
        load.wait()

    @pl.loop(0, ROWS // 32)
    def _(i):
        rows = hbuf[pl.ds(i * 32, 32), :].astype(F32)
        inv = lax.rsqrt(jnp.mean(rows * rows, axis=1, keepdims=True) + 1e-06)
        normed = (rows * inv * gain[...]).astype(BF16)
        for a in range(8):
            x[a, pl.ds(3 * ROWS + i * 32, 32), :] = normed[:, a * GROUP:(a + 1) * GROUP]

    for g in range(8):
        token_far(g).start()
    send_across(1)
    for g in range(8):
        token_near(g).start()

    def up_product(g, part, n, half):
        y, z = ORDER[0][g]
        for dx in range(4):
            need(0, half, (dx, y, z))
        if (g, part) not in fed:
            fed.add((g, part))
            (token_near(g) if part else token_relay(g)).wait_recv()
        a, wide = group(0, g), pl.ds(half * CHUNK, CHUNK)

        @pl.loop(0, 2)
        def _(i):
            rows = pl.ds(pl.multiple_of((2 * part + i) * ROWS, ROWS), ROWS)
            total = jnp.dot(x[a, rows, :], w[0, columns(a), wide], preferred_element_type=F32)
            if n > 0:
                total = total + acc[half, rows, :]
            if n < 7:
                acc[half, rows, :] = total
            else:
                act[rows, wide] = jnp.square(jnp.maximum(total * up_scale[:, wide], 0.0)).astype(BF16)

    def mine(a):
        return acc.at[0, pl.ds(pl.multiple_of((a % 4) * ROWS, ROWS), ROWS), columns(a // 4)]

    def products(first, a, g):
        @pl.loop(0, 2)
        def _(i):
            rows = pl.ds(pl.multiple_of((2 * first + i) * ROWS, ROWS), ROWS)
            part = lax.dot_general(act[rows, :], w[1, columns(a), :], (((1,), (1,)), ((), ())), preferred_element_type=F32)
            own[first, i] = part

            @pl.when(i == 0)
            def _():
                pbuf[g, first] = part.astype(BF16)
                near_part(g, first).start()

    def down_far(g):
        need_group(1, g)
        products(0, group(1, g), g)

    def sum_far(g):
        near_part(g, 0).wait_recv()
        zbuf[g] = (own[0, 1] + sibp[g, 0].astype(F32)).astype(BF16)
        far_part(g).start()

    def down_near(g):
        products(1, group(1, g), g)

    def output_sum(g):
        near_part(g, 1).wait_recv()
        mine(group(1, g))[...] = own[1, 1] + sibp[g, 1].astype(F32)

    def output(g):
        a = group(1, g, 1)
        far_part(g).wait_recv()
        out[:, columns(a)] = ((mine(a)[...] + zrecv[g].astype(F32)) * down_scale[:, columns(a)]).astype(BF16)

    for step in plan:
        kind, arg = step[0], step[1]
        if kind == 0:
            send(arg, step[2], step[3:6], step[6])
        elif kind == 1:
            token_far_in(arg).wait_recv()
            token_relay(arg).start()
        elif kind == 2:
            up_product(arg, *step[2:])
        elif kind == 3:
            down_far(arg)
        elif kind == 4:
            sum_far(arg)
        elif kind == 5:
            down_near(arg)
        elif kind == 6:
            output_sum(arg)
        else:
            output(arg)

    for phase in range(2):
        sent = w.at[phase, pl.ds(0, 31 * BLOCK), :]
        remote(sent, sent, ag_send.at[phase], ag_recv.at[0], sibling).wait_send()
    for i in range(3):
        sent = x.at[:, pl.ds(0, ROWS)]
        remote(sent, sent, tok_send.at[i], tok_recv.at[0, 0], sibling).wait_send()
    remote(sibp, sibp, par_send.at[0], par_recv.at[0, 0], sibling).wait_send()
    remote(zbuf, zbuf, par_send.at[1], par_recv.at[0, 0], sibling).wait_send()


def body(hidden_in, norm_gain, up_weight, up_scale, down_weight, down_scale):
    vmem, anywhere = pl.BlockSpec(memory_space=pltpu.VMEM), pl.BlockSpec(memory_space=pl.ANY)
    dma = pltpu.SemaphoreType.DMA
    return pl.pallas_call(
        kernel,
        out_shape=pltpu.VMEM((ROWS, D), BF16),
        in_specs=[anywhere] * 6,
        out_specs=vmem,
        scratch_shapes=[
            pltpu.VMEM((1, D), F32),
            pltpu.VMEM((1, Q), F32),
            pltpu.VMEM((1, D), F32),
            pltpu.VMEM((ROWS, D), BF16),
            pltpu.VMEM((2, BLOCK, Q), F32),
            pltpu.VMEM((2, BLOCK, Q), F32),
            pltpu.VMEM((2, BLOCK, Q), BF16),
            pltpu.VMEM((2, D, Q), BF16),
            pltpu.VMEM((8, 4 * ROWS, GROUP), BF16),
            pltpu.VMEM((Q // WIDE, 4 * ROWS, WIDE), F32),
            pltpu.VMEM((4 * ROWS, Q), BF16),
            pltpu.VMEM((8, 2, ROWS, GROUP), BF16),
            pltpu.VMEM((8, 2, ROWS, GROUP), BF16),
            pltpu.VMEM((2, 2, ROWS, GROUP), F32),
            pltpu.VMEM((8, ROWS, GROUP), BF16),
            pltpu.VMEM((8, ROWS, GROUP), BF16),
            dma((8,)),
            dma((2,)),
            dma((CHUNKS * 64,)),
            dma((3,)),
            dma((3, 8)),
            dma((2,)),
            dma((3, 8)),
        ],
        compiler_params=pltpu.CompilerParams(collective_id=0, has_side_effects=True, vmem_limit_bytes=63000000),
        name="ffn",
    )(hidden_in, norm_gain.reshape(1, -1), up_weight, up_scale.reshape(1, -1), down_weight.T, down_scale.reshape(1, -1))


def solution(mesh):
    placed = (P(("rep", "fs", "tp"), None), P(), P("fs", "tp"), P("tp"), P("tp", "fs"), P())
    return jax.shard_map(
        body, mesh=mesh, in_specs=placed, out_specs=P(("rep", "fs", "tp"), None), check_vma=False
    )
```
